32 devices in a mesh: ep: 8 (over z, x), tp: 4 (over y, core).
Axes of the slice: x: 2, y: 2, z: 4, core: 2. Of those that a mesh axis runs over, the one named last changes fastest.
Arguments:
- tokens: bfloat16 [32, 2048], P('ep'), may hold values from -6 to 6
- norm_gain: bfloat16 [2048], replicated, may hold values from 0.099609375 to 1.8984375
- in_weight: bfloat16 [2048, 1024], P(None, 'tp'), may hold values from -0.125 to 0.125
- decay_rate: float32 [64, 64], P('tp'), may hold values from 0.05 to 1
- frequency: float32 [64, 64], P('tp'), may hold values from -3 to 3
- log_step: float32 [64], P('tp'), may hold values from -2.3 to 0.7
- input_real: float32 [64, 64, 16], P('tp'), may hold values from -1.75 to 1.75
- input_imag: float32 [64, 64, 16], P('tp'), may hold values from -1.75 to 1.75
- output_real: float32 [64, 16, 64], P('tp'), may hold values from -0.5 to 0.5
- output_imag: float32 [64, 16, 64], P('tp'), may hold values from -0.5 to 0.5
- skip_gain: float32 [1024], P('tp'), may hold values from -3 to 3
- state_real: float32 [32, 64, 64], P('ep', 'tp'), may hold values from -6 to 6
- state_imag: float32 [32, 64, 64], P('ep', 'tp'), may hold values from -6 to 6
- out_weight: bfloat16 [1024, 2048], P('tp'), may hold values from -0.1875 to 0.1875
- ffn_gain: bfloat16 [2048], replicated, may hold values from 0.099609375 to 1.8984375
- expert_ids: int32 [32, 2], replicated, may hold values from 0 to 7, all different within a row; in each aligned block of 4 rows (0 to 3, 4 to 7, ...) at most 2 rows name the same one
- route_weights: float32 [32, 2], P('ep'), may hold values from 0.2 to 1
- gate_weight: bfloat16 [2048, 65536], P(None, ('ep', 'tp')), may hold values from -0.125 to 0.125
- up_weight: bfloat16 [2048, 65536], P(None, ('ep', 'tp')), may hold values from -0.125 to 0.125
- down_weight: bfloat16 [65536, 2048], P('ep', 'tp'), may hold values from -0.0625 to 0.0625
Outputs:
- mixed: bfloat16 [32, 2048], P('ep', 'tp')
- new_real: float32 [32, 64, 64], P('ep', 'tp')
- new_imag: float32 [32, 64, 64], P('ep', 'tp')
The draws below stay inside these ranges and needn't reach their ends.
Inputs may be any that keep to these rules, and one draw needn't show every extreme that they name: `expert_ids`: the 2 experts of a row differ. In each aligned block of 4 rows (the rows of one index of ep) no expert is named by more than 2 rows, and in some blocks one expert is named by exactly 2 rows.
All inputs are finite; a program needn't handle non-finite values.
Results may differ from the reference program's by a relative error of at most 0.007.
Values may be sent and summed in bfloat16 or wider, within the bound.
No kernel may reach another device: no remote copies, remote signals or barrier semaphores. Data moves between devices by JAX's collectives and lax.ppermute only.
A program may use at most 64 MiB of HBM per device.

```python
import math
import jax
import jax.numpy as jnp
import numpy as np
from jax import lax

D = 2048
S5W = 1024
GROUP = 16
STATE = 64
EXPERTS = 8
TOP = 2
FF = 8192
SEQ_DEV = 4
GROUPS = 64
CAP = 2
TOKENS = 32
SPAN = 1
N_EP = 8


def block_levels(stream_key, dims, cuts, low, largest):
    factor_of, own = 1.0, jax.random.fold_in(stream_key, 6)
    for position, shards_of in cuts:
        steps = jnp.exp(jax.random.uniform(jax.random.fold_in(own, position), (shards_of,), jnp.float32, low / len(cuts), largest / len(cuts)))
        factor_of = factor_of * jnp.repeat(steps, dims[position] // shards_of).reshape([-1 if axis == position else 1 for axis in range(len(dims))])
    return factor_of


def assign_block(key, own, number, rows, amount, top, most, slope):
    sequence = jax.random.permutation(key, amount)
    packed, ordinary = load_shares(amount, rows * top, most, slope, True), load_shares(amount, rows * top, most, slope, False)
    places = jnp.arange(amount)

    def named(sizes, turn):
        used = int((sizes > 0).sum())
        fixed = max(1, used // 4)
        moved = fixed + (places - fixed + turn * (used - fixed)) % max(1, amount - fixed)
        return jnp.zeros((amount,), jnp.int32).at[sequence[jnp.where(places < fixed, places, moved)]].set(jnp.asarray(sizes, jnp.int32))

    sizes = jnp.where(number % 4 == 0, named(packed, number // 4), named(ordinary, number - number // 4 - 1))
    mixed = jax.random.permutation(jax.random.fold_in(own, 3), amount)
    donor, taker = mixed[0:amount // 2 * 2:2], mixed[1:amount // 2 * 2:2]
    slack = jnp.minimum(sizes[donor] - 1, most - sizes[taker]) // 2
    slack = jnp.where((donor == sequence[0]) | (taker == sequence[0]) | (sizes[taker] == 0), 0, jnp.maximum(slack, 0))
    moved = jax.random.randint(jax.random.fold_in(own, 4), (amount // 2,), 0, 1 << 20) % (slack + 1)
    sizes = sizes.at[donor].add(-moved).at[taker].add(moved)
    members = jnp.searchsorted(jnp.cumsum(sizes), jnp.arange(rows * top), side="right").astype(jnp.int32)
    grid = members.reshape(top, rows).T
    grid = grid[jax.random.permutation(jax.random.fold_in(own, 1), rows)]
    turn = jax.random.randint(jax.random.fold_in(own, 2), (rows, 1), 0, top)
    return jnp.take_along_axis(grid, (jnp.arange(top)[None, :] + turn) % top, axis=1)


def load_shares(amount, total, bound, slope, full):
    loads = [(1 << 20) // math.isqrt(grade ** slope) + 1 for grade in range(1, amount + 1)]
    largest = bound if full else min(bound, max(-(-total // amount), total * loads[0] // sum(loads)))
    least = 1 if total - largest >= amount - 1 else 0
    counts, rest = [largest] + [least] * (amount - 1), total - largest - least * (amount - 1)
    while rest > 0:
        candidates = [i for i in range(1, amount) if counts[i] < largest] or [i for i in range(1, amount) if counts[i] < bound]
        pool, left = sum([loads[i] for i in candidates]), rest
        for i in candidates:
            more = min(bound - counts[i], max(1, left * loads[i] // pool), rest)
            counts[i] = counts[i] + more
            rest = rest - more
    return np.array(counts)


def bell_draw(stream_key, shape, spread, most, cuts=(), held_as=jnp.bfloat16):
    entries = jax.random.normal(stream_key, shape, jnp.float32) * spread
    if len(cuts) > 0:
        entries = block_levels(stream_key, shape, cuts, -0.22, 0.18) * entries
    return jnp.clip(entries, min=-most, max=most).astype(held_as)


def setup_inputs(seed: int = 0) -> dict:
    splits = jax.random.split(jax.random.key(seed), 21)
    tokens = bell_draw(splits[0], (TOKENS, D), 1.0, 6.0, ((0, 8),))
    norm_gain = jnp.clip(1.0 + 0.18 * jax.random.normal(splits[1], (D,), jnp.float32), 0.099609375, 1.8984375).astype(jnp.bfloat16)
    in_weight = bell_draw(splits[2], (D, S5W), D ** -0.5, 0.125, ((1, 4),))
    decay_rate = jnp.clip(jnp.exp(math.log(1.0) - 2.9957323 * jax.random.uniform(splits[3], (GROUPS, STATE), jnp.float32) ** block_levels(splits[3], (GROUPS, STATE), ((0, 4),), -0.2, 0.2)), 0.05, 1.0)
    frequency = jnp.clip(jax.random.uniform(splits[4], (GROUPS, STATE), jnp.float32, -3.0, 3.0) * block_levels(splits[4], (GROUPS, STATE), ((0, 4),), -0.4, 0.0), -3.0, 3.0)
    log_step = jnp.clip(-2.3 + 3 * jax.random.uniform(splits[5], (GROUPS,), jnp.float32) ** block_levels(splits[5], (GROUPS,), ((0, 4),), -0.2, 0.2), -2.3, 0.7)
    input_real = bell_draw(splits[6], (GROUPS, STATE, GROUP), 0.3, 1.75, ((0, 4),), jnp.float32)
    input_imag = bell_draw(splits[7], (GROUPS, STATE, GROUP), 0.3, 1.75, ((0, 4),), jnp.float32)
    output_real = bell_draw(splits[8], (GROUPS, GROUP, STATE), (2 * STATE) ** -0.5, 0.5, ((0, 4),), jnp.float32)
    output_imag = bell_draw(splits[9], (GROUPS, GROUP, STATE), (2 * STATE) ** -0.5, 0.5, ((0, 4),), jnp.float32)
    skip_gain = bell_draw(splits[10], (S5W,), 0.5, 3.0, ((0, 4),), jnp.float32)
    state_real = bell_draw(splits[11], (TOKENS, GROUPS, STATE), 1.0, 6.0, ((0, 8), (1, 4)), jnp.float32)
    state_imag = bell_draw(splits[12], (TOKENS, GROUPS, STATE), 1.0, 6.0, ((0, 8), (1, 4)), jnp.float32)
    out_weight = bell_draw(splits[13], (S5W, D), S5W ** -0.5, 0.1875, ((0, 4),))
    ffn_gain = jnp.clip(1.0 + 0.18 * jax.random.normal(splits[14], (D,), jnp.float32), 0.099609375, 1.8984375).astype(jnp.bfloat16)
    expert_ids_keys = jax.random.split(jax.random.fold_in(splits[15], 1), TOKENS // SEQ_DEV)
    expert_ids_turns = jax.random.permutation(jax.random.fold_in(splits[15], 3), TOKENS // SEQ_DEV)
    expert_ids = jax.vmap(lambda own, number: assign_block(jax.random.fold_in(splits[15], 2), own, number, SEQ_DEV, EXPERTS, TOP, CAP, 2))(expert_ids_keys, expert_ids_turns).reshape((TOKENS, TOP))
    route_weights = jnp.clip(0.2 + 0.8 * jax.random.uniform(splits[16], (TOKENS, TOP), jnp.float32) ** block_levels(splits[16], (TOKENS, TOP), ((0, 8),), -0.2, 0.2), 0.2, 1.0)
    gate_weight = bell_draw(splits[17], (D, EXPERTS * FF), D ** -0.5, 0.125, ((1, 32),))
    up_weight = bell_draw(splits[18], (D, EXPERTS * FF), D ** -0.5, 0.125, ((1, 32),))
    down_weight = bell_draw(splits[19], (EXPERTS * FF, D), FF ** -0.5, 0.0625, ((0, 8), (1, 4)))
    return {"tokens": tokens, "norm_gain": norm_gain, "in_weight": in_weight, "decay_rate": decay_rate, "frequency": frequency, "log_step": log_step, "input_real": input_real, "input_imag": input_imag, "output_real": output_real, "output_imag": output_imag, "skip_gain": skip_gain, "state_real": state_real, "state_imag": state_imag, "out_weight": out_weight, "ffn_gain": ffn_gain, "expert_ids": expert_ids, "route_weights": route_weights, "gate_weight": gate_weight, "up_weight": up_weight, "down_weight": down_weight}


EPSILON = 1e-06

def rms_scale(values, gain):
    floats = values.astype(jnp.float32)
    return floats * lax.rsqrt(lax.optimization_barrier(jnp.mean(floats * floats, axis=-1, keepdims=True)) + EPSILON) * gain.astype(jnp.float32)

def discretize(decay_rate, frequency, log_step, input_real, input_imag):
    step_size = jnp.exp(log_step)[:, None]
    lam_real = -decay_rate
    magnitude = jnp.exp(lam_real * step_size)
    turned = frequency * step_size
    bar_real = magnitude * jnp.cos(turned)
    bar_imag = magnitude * jnp.sin(turned)
    denom = lam_real * lam_real + frequency * frequency
    minus_one = bar_real - 1.0
    factor_real = (minus_one * lam_real + bar_imag * frequency) / denom
    factor_imag = (bar_imag * lam_real - minus_one * frequency) / denom
    b_real = factor_real[..., None] * input_real - factor_imag[..., None] * input_imag
    b_imag = factor_real[..., None] * input_imag + factor_imag[..., None] * input_real
    return (bar_real, bar_imag, b_real, b_imag)

def state_update(projected, state_real, state_imag, decay_rate, frequency, log_step, input_real, input_imag, output_real, output_imag, skip_gain):
    bar_real, bar_imag, b_real, b_imag = discretize(decay_rate, frequency, log_step, input_real, input_imag)
    count, groups, _ = state_real.shape
    high = lax.Precision.HIGHEST
    grouped = projected.astype(jnp.float32).reshape(count, groups, -1)
    drive_real = jnp.einsum('sgp,gnp->sgn', grouped, b_real, precision=high)
    drive_imag = jnp.einsum('sgp,gnp->sgn', grouped, b_imag, precision=high)
    new_real = bar_real * state_real - bar_imag * state_imag + drive_real
    new_imag = bar_real * state_imag + bar_imag * state_real + drive_imag
    readout = jnp.einsum('sgn,gpn->sgp', new_real, output_real, precision=high) - jnp.einsum('sgn,gpn->sgp', new_imag, output_imag, precision=high)
    readout = readout.reshape(count, -1) + skip_gain * grouped.reshape(count, -1)
    return (jax.nn.gelu(readout).astype(jnp.bfloat16), new_real, new_imag)

def reference(tokens, norm_gain, in_weight, decay_rate, frequency, log_step, input_real, input_imag, output_real, output_imag, skip_gain, state_real, state_imag, out_weight, ffn_gain, expert_ids, route_weights, gate_weight, up_weight, down_weight):
    normed_in = rms_scale(tokens, norm_gain).astype(jnp.bfloat16)
    projected = jnp.dot(normed_in, in_weight, preferred_element_type=jnp.float32).astype(jnp.bfloat16)
    activated, new_real, new_imag = state_update(projected, state_real, state_imag, decay_rate, frequency, log_step, input_real, input_imag, output_real, output_imag, skip_gain)
    delta = jnp.dot(activated, out_weight, preferred_element_type=jnp.float32)
    hidden_state = (tokens.astype(jnp.float32) + delta).astype(jnp.bfloat16)
    normed = rms_scale(hidden_state, ffn_gain).astype(jnp.bfloat16)
    limit = min(TOKENS, N_EP * CAP)
    piece = FF // SPAN

    def expert_block(carry, expert):
        hits = expert_ids == expert
        row_weight = lax.optimization_barrier(jnp.sum(jnp.where(hits, route_weights, 0.0), axis=1))
        used = jnp.any(hits, axis=1)
        indices = jnp.nonzero(used, size=limit, fill_value=0)[0].astype(jnp.int32)
        valid = jnp.arange(limit, dtype=jnp.int32) < jnp.sum(used.astype(jnp.int32))
        chosen = normed[indices]
        start = (expert * FF).astype(jnp.int32)
        gate_cols = lax.dynamic_slice_in_dim(gate_weight, start, FF, 1)
        up_cols = lax.dynamic_slice_in_dim(up_weight, start, FF, 1)
        down_rows = lax.dynamic_slice_in_dim(down_weight, start, FF, 0)
        gate_pre = jnp.dot(chosen, gate_cols, preferred_element_type=jnp.float32)
        up_pre = jnp.dot(chosen, up_cols, preferred_element_type=jnp.float32)
        expert_hidden = (jax.nn.silu(gate_pre) * up_pre).astype(jnp.bfloat16)

        def one_piece(index):
            first = (index * piece).astype(jnp.int32)
            units = lax.dynamic_slice_in_dim(expert_hidden, first, piece, 1)
            rows = lax.dynamic_slice_in_dim(down_rows, first, piece, 0)
            part = jnp.dot(units, rows, preferred_element_type=jnp.float32).astype(jnp.bfloat16)
            return lax.optimization_barrier(part).astype(jnp.float32)
        pieces = lax.map(one_piece, jnp.arange(SPAN, dtype=jnp.int32))
        expert_out = lax.optimization_barrier(jnp.sum(pieces, axis=0))
        scale = jnp.where(valid, row_weight[indices], 0.0)
        return (carry.at[indices].add(scale[:, None] * expert_out), None)
    routed, _ = lax.scan(expert_block, jnp.zeros(normed.shape, jnp.float32), jnp.arange(EXPERTS, dtype=jnp.int32))
    mixed = (hidden_state.astype(jnp.float32) + routed).astype(jnp.bfloat16)
    return (mixed, new_real, new_imag)
```

```python
import jax
import jax.numpy as jnp
from jax import lax
from jax.experimental import pallas as pl
from jax.experimental.pallas import tpu as pltpu
from jax.sharding import PartitionSpec as P

EXPERTS = 8
EPSILON = 1e-06
F32 = jnp.float32
BF16 = jnp.bfloat16
MIB = 1 << 20
PIECES = 4


def dot(a, b, contract=((1,), (0,))):
    return lax.dot_general(a, b, (contract, ((), ())), preferred_element_type=F32)


def split_high_low(values):
    high = values.astype(BF16)
    return high, (values - high.astype(F32)).astype(BF16)


def rms_norm(floats, gain):
    scale = lax.rsqrt(jnp.mean(floats * floats, axis=-1, keepdims=True) + EPSILON)
    return (floats * scale * gain.astype(F32)).astype(BF16)


def repeat_rows(values, count):
    rows = [
        jnp.broadcast_to(values[s : s + 1], (count, values.shape[1]))
        for s in range(values.shape[0])
    ]
    return jnp.concatenate(rows, axis=0)


def slot_tables(base, ids, weights, count, slots):
    total = ids.shape[1]
    pick = (total, count)
    own = lax.broadcasted_iota(jnp.int32, pick, 0) == base + lax.broadcasted_iota(
        jnp.int32, pick, 1
    )
    own_ids = dot(ids.astype(F32).astype(BF16), own.astype(F32).astype(BF16))
    shape = (EXPERTS * slots, count)
    row = lax.broadcasted_iota(jnp.int32, shape, 0)
    expert = (row // slots).astype(F32)
    place = (row % slots).astype(F32)
    hits = jnp.zeros(shape, F32)
    scaled = jnp.zeros(shape, F32)
    for k in range(ids.shape[0]):
        same = jnp.broadcast_to(own_ids[k : k + 1], shape) == expert
        hits = hits + jnp.where(same, 1.0, 0.0)
        scaled = scaled + jnp.where(same, jnp.broadcast_to(weights[k : k + 1], shape), 0.0)
    earlier = (count, count)
    upper = lax.broadcasted_iota(jnp.int32, earlier, 0) < lax.broadcasted_iota(
        jnp.int32, earlier, 1
    )
    before = dot(hits.astype(BF16), upper.astype(F32).astype(BF16))
    placed = before == place
    return jnp.where(placed, hits, 0.0), jnp.where(placed, scaled, 0.0)


def as_row(values):
    rows = values.astype(F32)
    return jnp.concatenate([rows[j : j + 1] for j in range(rows.shape[0])], axis=1)


MIXER_INPUTS = 17


def mixer_kernel(base, *refs):
    sources, refs = refs[:MIXER_INPUTS], refs[MIXER_INPUTS:]
    partial, new_real, new_imag, kept_tokens, kept_gain, select, table = refs[:7]
    buffers, sems = refs[7:-1], refs[-1]
    copies = [
        pltpu.make_async_copy(source, buffer, sems.at[i])
        for i, (source, buffer) in enumerate(zip(sources, buffers))
    ]
    for copy in copies:
        copy.start()
    (
        tokens,
        norm_gain,
        in_weight,
        decay_rate,
        frequency,
        log_step,
        input_real,
        input_imag,
        output_real,
        output_imag,
        skip_gain,
        state_real,
        state_imag,
        ffn_gain,
        ids,
        weights,
        out_weight,
    ) = buffers
    for copy in copies[:-1]:
        copy.wait()
    kept_tokens[...] = tokens[...]
    kept_gain[...] = as_row(ffn_gain[...])
    selected, scaled = slot_tables(
        base[0], ids[...], weights[...], tokens.shape[0], select.shape[0] // EXPERTS
    )
    select[...] = selected
    table[...] = scaled
    count = tokens.shape[0]
    groups, states = decay_rate.shape
    channels = in_weight.shape[1]
    width = channels // groups
    normed = rms_norm(tokens[...].astype(F32), as_row(norm_gain[...]))
    projected = dot(normed, in_weight[...]).astype(BF16).astype(F32)
    shape = (count * groups, channels)
    row_group = lax.broadcasted_iota(jnp.int32, shape, 0) % groups
    own_group = row_group == lax.broadcasted_iota(jnp.int32, shape, 1) // width
    spread = jnp.where(own_group, repeat_rows(projected, groups), 0.0).astype(BF16)
    inputs = jnp.concatenate([input_real[...], input_imag[...]], axis=1)
    inputs_high, inputs_low = split_high_low(inputs)
    driven = dot(spread, inputs_high) + dot(spread, inputs_low)
    driven_real, driven_imag = driven[:, :states], driven[:, states:]

    square = (groups, groups)
    diagonal = lax.broadcasted_iota(jnp.int32, square, 0) == lax.broadcasted_iota(
        jnp.int32, square, 1
    )
    step_size = jnp.exp(
        jnp.sum(
            jnp.where(diagonal, jnp.broadcast_to(log_step[...], square), 0.0),
            axis=1,
            keepdims=True,
        )
    )
    lam_real = -decay_rate[...]
    lam_imag = frequency[...]
    magnitude = jnp.exp(lam_real * step_size)
    turned = lam_imag * step_size
    bar_real = magnitude * jnp.cos(turned)
    bar_imag = magnitude * jnp.sin(turned)
    denom = lam_real * lam_real + lam_imag * lam_imag
    minus_one = bar_real - 1.0
    factor_real = (minus_one * lam_real + bar_imag * lam_imag) / denom
    factor_imag = (bar_imag * lam_real - minus_one * lam_imag) / denom
    bar_real, bar_imag, factor_real, factor_imag = (
        jnp.concatenate([v] * count, axis=0)
        for v in (bar_real, bar_imag, factor_real, factor_imag)
    )
    old_real, old_imag = state_real[...], state_imag[...]
    fresh_real = (
        bar_real * old_real
        - bar_imag * old_imag
        + factor_real * driven_real
        - factor_imag * driven_imag
    )
    fresh_imag = (
        bar_real * old_imag
        + bar_imag * old_real
        + factor_real * driven_imag
        + factor_imag * driven_real
    )
    new_real[...] = fresh_real
    new_imag[...] = fresh_imag

    fresh_high, fresh_low = split_high_low(jnp.concatenate([fresh_real, fresh_imag], axis=1))
    out_high, out_low = split_high_low(
        jnp.concatenate([output_real[...], -output_imag[...]], axis=1)
    )
    across = ((1,), (1,))
    read = (
        dot(fresh_high, out_high, across)
        + dot(fresh_low, out_high, across)
        + dot(fresh_high, out_low, across)
    )
    read = jnp.where(own_group, read, 0.0)
    read = jnp.concatenate(
        [
            jnp.sum(read[s * groups : (s + 1) * groups], axis=0, keepdims=True)
            for s in range(count)
        ],
        axis=0,
    )
    activated = jax.nn.gelu(read + skip_gain[...] * projected).astype(BF16)
    copies[-1].wait()
    partial[...] = dot(activated, out_weight[...])


def prefetch_kernel(order, gate, up, gate_copy, up_copy, sems):
    del order
    pairs = []
    for source, target in ((gate, gate_copy), (up, up_copy)):
        part = source.shape[0] // PIECES
        for j in range(PIECES):
            rows = pl.ds(j * part, part)
            pairs.append((source.at[rows], target.at[rows]))
    copies = [pltpu.make_async_copy(a, b, sems.at[i]) for i, (a, b) in enumerate(pairs)]
    for copy in copies:
        copy.start()
    for copy in copies:
        copy.wait()


def dispatch_kernel(*refs):
    shares, (tokens, gain, select, _, _, outgoing, hidden) = refs[:-7], refs[-7:]
    slots = outgoing.shape[1]
    delta = shares[0][...]
    for share in shares[1:]:
        delta = delta + share[...]
    hidden_state = (tokens[...].astype(F32) + delta).astype(BF16)
    hidden[...] = hidden_state
    normed = rms_norm(hidden_state.astype(F32), gain[...])
    sent = dot(select[...].astype(BF16), normed).astype(BF16)
    for x in range(EXPERTS):
        outgoing[x] = sent[x * slots : (x + 1) * slots]


def hidden_kernel(received, gate, up, hidden):
    rows = jnp.concatenate([received[x] for x in range(received.shape[0])], axis=0)
    gate_pre = dot(rows, gate[...])
    up_pre = dot(rows, up[...])
    hidden[...] = (jax.nn.silu(gate_pre) * up_pre).astype(BF16)


def down_kernel(hidden, down, out):
    units = hidden.shape[2]
    total = dot(hidden[0], down[:units])
    for j in range(1, hidden.shape[0]):
        total = total + dot(hidden[j], down[j * units : (j + 1) * units])
    rounded = total.astype(BF16)
    slots = out.shape[1]
    for x in range(out.shape[0]):
        out[x] = rounded[x * slots : (x + 1) * slots]


def combine_kernel(start, returned, table, hidden, mixed):
    quarter = mixed.shape[1]
    rows = jnp.concatenate([returned[x] for x in range(returned.shape[0])], axis=0)
    routed = lax.dot_general(
        table[...],
        rows.astype(F32),
        (((0,), (0,)), ((), ())),
        precision=lax.Precision.HIGHEST,
        preferred_element_type=F32,
    )
    first = pl.multiple_of(start[0], 128)
    residual = hidden[:, pl.ds(first, quarter)].astype(F32)
    mixed[...] = (residual + routed).astype(BF16)


def call(kernel, out, args, limit, scalars=0):
    specs = [pl.BlockSpec(memory_space=pltpu.SMEM)] * scalars
    specs = specs + [pl.BlockSpec(memory_space=pltpu.VMEM)] * (len(args) - scalars)
    return pl.pallas_call(
        kernel,
        out_shape=out,
        in_specs=specs,
        compiler_params=pltpu.CompilerParams(vmem_limit_bytes=limit * MIB),
    )(*args)


def shards(
    tokens,
    norm_gain,
    in_weight,
    decay_rate,
    frequency,
    log_step,
    input_real,
    input_imag,
    output_real,
    output_imag,
    skip_gain,
    state_real,
    state_imag,
    out_weight,
    ffn_gain,
    expert_ids,
    route_weights,
    gate_weight,
    up_weight,
    down_weight,
):
    count, width = tokens.shape
    groups, states = decay_rate.shape
    channels = in_weight.shape[1]
    quarter = down_weight.shape[1]
    flat_state = (count * groups, states)
    struct = jax.ShapeDtypeStruct
    slots = count // 2
    base = jnp.reshape(lax.axis_index("ep") * count, (1,)).astype(jnp.int32)
    start = jnp.reshape(lax.axis_index("tp") * quarter, (1,)).astype(jnp.int32)
    sources = (
        tokens,
        norm_gain.reshape(-1, 128),
        in_weight,
        decay_rate,
        frequency,
        log_step[None],
        jnp.swapaxes(input_real, 1, 2).reshape(channels, states),
        jnp.swapaxes(input_imag, 1, 2).reshape(channels, states),
        output_real.reshape(channels, states),
        output_imag.reshape(channels, states),
        skip_gain[None],
        state_real.reshape(flat_state),
        state_imag.reshape(flat_state),
        ffn_gain.reshape(-1, 128),
        expert_ids.T,
        route_weights.T,
        out_weight,
    )
    hbm = pl.BlockSpec(memory_space=pltpu.HBM)
    vmem = pl.BlockSpec(memory_space=pltpu.VMEM)
    smem = pl.BlockSpec(memory_space=pltpu.SMEM)
    table_shape = struct((EXPERTS * slots, count), F32)
    partial, new_real, new_imag, kept_tokens, kept_gain, select, table = pl.pallas_call(
        mixer_kernel,
        out_shape=(
            struct((count, width), F32),
            struct(flat_state, F32),
            struct(flat_state, F32),
            struct((count, width), BF16),
            struct((1, width), F32),
            table_shape,
            table_shape,
        ),
        in_specs=[smem] + [hbm] * len(sources),
        scratch_shapes=[pltpu.VMEM(v.shape, v.dtype) for v in sources]
        + [pltpu.SemaphoreType.DMA((len(sources),))],
        compiler_params=pltpu.CompilerParams(vmem_limit_bytes=10 * MIB),
    )(base, *[pltpu.with_memory_space_constraint(v, pltpu.HBM) for v in sources])
    ways = lax.axis_size("tp")
    shares = [partial] + [
        lax.ppermute(partial, "tp", [(i, (i + k) % ways) for i in range(ways)])
        for k in range(1, ways)
    ]
    gate_here, up_here = pl.pallas_call(
        prefetch_kernel,
        out_shape=(
            struct(gate_weight.shape, BF16),
            struct(up_weight.shape, BF16),
        ),
        in_specs=[vmem, hbm, hbm],
        out_specs=(vmem, vmem),
        scratch_shapes=[pltpu.SemaphoreType.DMA((2 * PIECES,))],
        compiler_params=pltpu.CompilerParams(vmem_limit_bytes=1 * MIB),
    )(
        select,
        pltpu.with_memory_space_constraint(gate_weight, pltpu.HBM),
        pltpu.with_memory_space_constraint(up_weight, pltpu.HBM),
    )
    outgoing, hidden_state = call(
        dispatch_kernel,
        (struct((EXPERTS, slots, width), BF16), struct((count, width), BF16)),
        (*shares, kept_tokens, kept_gain, select, gate_here, up_here),
        4,
    )
    span = lax.axis_size("ep") // EXPERTS
    if span > 1:
        outgoing = jnp.repeat(outgoing, span, axis=0)
    received = lax.all_to_all(outgoing, "ep", split_axis=0, concat_axis=0, tiled=True)
    peers = received.shape[0]
    hidden = call(
        hidden_kernel,
        struct((peers * slots, gate_weight.shape[1]), BF16),
        (received, gate_here, up_here),
        4,
    )
    out = call(
        down_kernel,
        struct((peers, slots, quarter), BF16),
        (lax.all_gather(hidden, "tp"), down_weight),
        6,
    )
    returned = lax.all_to_all(out, "ep", split_axis=0, concat_axis=0, tiled=True)
    if span > 1:
        returned = returned.astype(F32).reshape(EXPERTS, span, slots, quarter).sum(axis=1)
    mixed = call(
        combine_kernel,
        struct((count, quarter), BF16),
        (start, returned, table, hidden_state),
        2,
        1,
    )
    shape = state_real.shape
    return (mixed, new_real.reshape(shape), new_imag.reshape(shape))

def solution(mesh):
    in_specs = (
        P("ep", None),
        P(),
        P(None, "tp"),
        P("tp", None),
        P("tp", None),
        P("tp"),
        P("tp", None, None),
        P("tp", None, None),
        P("tp", None, None),
        P("tp", None, None),
        P("tp"),
        P("ep", "tp", None),
        P("ep", "tp", None),
        P("tp", None),
        P(),
        P(),
        P("ep", None),
        P(None, ("ep", "tp")),
        P(None, ("ep", "tp")),
        P("ep", "tp"),
    )
    out_specs = (P("ep", "tp"), P("ep", "tp", None), P("ep", "tp", None))
    return jax.shard_map(shards, mesh=mesh, in_specs=in_specs, out_specs=out_specs, check_vma=False)
```

```python
import jax
import jax.numpy as jnp
from jax import lax
from jax.experimental import pallas as pl
from jax.experimental.pallas import tpu as pltpu
from jax.sharding import PartitionSpec as P

EXPERTS = 8
EPSILON = 1e-06
F32 = jnp.float32
BF16 = jnp.bfloat16
MIB = 1 << 20


def dot(a, b, contract=((1,), (0,))):
    return lax.dot_general(a, b, (contract, ((), ())), preferred_element_type=F32)


def split_high_low(values):
    high = values.astype(BF16)
    return high, (values - high.astype(F32)).astype(BF16)


def rms_norm(floats, gain):
    scale = lax.rsqrt(jnp.mean(floats * floats, axis=-1, keepdims=True) + EPSILON)
    return (floats * scale * gain.astype(F32)).astype(BF16)


def repeat_rows(values, count):
    rows = [
        jnp.broadcast_to(values[s : s + 1], (count, values.shape[1]))
        for s in range(values.shape[0])
    ]
    return jnp.concatenate(rows, axis=0)


def slot_tables(base, ids, weights, count, slots):
    total = ids.shape[1]
    pick = (total, count)
    own = lax.broadcasted_iota(jnp.int32, pick, 0) == base + lax.broadcasted_iota(
        jnp.int32, pick, 1
    )
    own_ids = dot(ids.astype(F32).astype(BF16), own.astype(F32).astype(BF16))
    shape = (EXPERTS * slots, count)
    row = lax.broadcasted_iota(jnp.int32, shape, 0)
    expert = (row // slots).astype(F32)
    place = (row % slots).astype(F32)
    hits = jnp.zeros(shape, F32)
    scaled = jnp.zeros(shape, F32)
    for k in range(ids.shape[0]):
        same = jnp.broadcast_to(own_ids[k : k + 1], shape) == expert
        hits = hits + jnp.where(same, 1.0, 0.0)
        scaled = scaled + jnp.where(same, jnp.broadcast_to(weights[k : k + 1], shape), 0.0)
    earlier = (count, count)
    upper = lax.broadcasted_iota(jnp.int32, earlier, 0) < lax.broadcasted_iota(
        jnp.int32, earlier, 1
    )
    before = dot(hits.astype(BF16), upper.astype(F32).astype(BF16))
    placed = before == place
    return jnp.where(placed, hits, 0.0), jnp.where(placed, scaled, 0.0)


def as_row(values):
    rows = values.astype(F32)
    return jnp.concatenate([rows[j : j + 1] for j in range(rows.shape[0])], axis=1)


MIXER_INPUTS = 17


def mixer_kernel(base, *refs):
    sources, refs = refs[:MIXER_INPUTS], refs[MIXER_INPUTS:]
    partial, new_real, new_imag, kept_tokens, kept_gain, select, table = refs[:7]
    buffers, sems = refs[7:-1], refs[-1]
    copies = [
        pltpu.make_async_copy(source, buffer, sems.at[i])
        for i, (source, buffer) in enumerate(zip(sources, buffers))
    ]
    for copy in copies:
        copy.start()
    (
        tokens,
        norm_gain,
        in_weight,
        decay_rate,
        frequency,
        log_step,
        input_real,
        input_imag,
        output_real,
        output_imag,
        skip_gain,
        state_real,
        state_imag,
        ffn_gain,
        ids,
        weights,
        out_weight,
    ) = buffers
    for copy in copies[:-1]:
        copy.wait()
    kept_tokens[...] = tokens[...]
    kept_gain[...] = as_row(ffn_gain[...])
    selected, scaled = slot_tables(
        base[0], ids[...], weights[...], tokens.shape[0], select.shape[0] // EXPERTS
    )
    select[...] = selected
    table[...] = scaled
    count = tokens.shape[0]
    groups, states = decay_rate.shape
    channels = in_weight.shape[1]
    width = channels // groups
    normed = rms_norm(tokens[...].astype(F32), as_row(norm_gain[...]))
    projected = dot(normed, in_weight[...]).astype(BF16).astype(F32)
    shape = (count * groups, channels)
    row_group = lax.broadcasted_iota(jnp.int32, shape, 0) % groups
    own_group = row_group == lax.broadcasted_iota(jnp.int32, shape, 1) // width
    spread = jnp.where(own_group, repeat_rows(projected, groups), 0.0).astype(BF16)
    inputs = jnp.concatenate([input_real[...], input_imag[...]], axis=1)
    inputs_high, inputs_low = split_high_low(inputs)
    driven = dot(spread, inputs_high) + dot(spread, inputs_low)
    driven_real, driven_imag = driven[:, :states], driven[:, states:]

    square = (groups, groups)
    diagonal = lax.broadcasted_iota(jnp.int32, square, 0) == lax.broadcasted_iota(
        jnp.int32, square, 1
    )
    step_size = jnp.exp(
        jnp.sum(
            jnp.where(diagonal, jnp.broadcast_to(log_step[...], square), 0.0),
            axis=1,
            keepdims=True,
        )
    )
    lam_real = -decay_rate[...]
    lam_imag = frequency[...]
    magnitude = jnp.exp(lam_real * step_size)
    turned = lam_imag * step_size
    bar_real = magnitude * jnp.cos(turned)
    bar_imag = magnitude * jnp.sin(turned)
    denom = lam_real * lam_real + lam_imag * lam_imag
    minus_one = bar_real - 1.0
    factor_real = (minus_one * lam_real + bar_imag * lam_imag) / denom
    factor_imag = (bar_imag * lam_real - minus_one * lam_imag) / denom
    bar_real, bar_imag, factor_real, factor_imag = (
        jnp.concatenate([v] * count, axis=0)
        for v in (bar_real, bar_imag, factor_real, factor_imag)
    )
    old_real, old_imag = state_real[...], state_imag[...]
    fresh_real = (
        bar_real * old_real
        - bar_imag * old_imag
        + factor_real * driven_real
        - factor_imag * driven_imag
    )
    fresh_imag = (
        bar_real * old_imag
        + bar_imag * old_real
        + factor_real * driven_imag
        + factor_imag * driven_real
    )
    new_real[...] = fresh_real
    new_imag[...] = fresh_imag

    fresh_high, fresh_low = split_high_low(jnp.concatenate([fresh_real, fresh_imag], axis=1))
    out_high, out_low = split_high_low(
        jnp.concatenate([output_real[...], -output_imag[...]], axis=1)
    )
    across = ((1,), (1,))
    read = (
        dot(fresh_high, out_high, across)
        + dot(fresh_low, out_high, across)
        + dot(fresh_high, out_low, across)
    )
    read = jnp.where(own_group, read, 0.0)
    read = jnp.concatenate(
        [
            jnp.sum(read[s * groups : (s + 1) * groups], axis=0, keepdims=True)
            for s in range(count)
        ],
        axis=0,
    )
    activated = jax.nn.gelu(read + skip_gain[...] * projected).astype(BF16)
    copies[-1].wait()
    partial[...] = dot(activated, out_weight[...])


def dispatch_kernel(gathered, tokens, gain, select, gate, up, outgoing, hidden):
    del gate, up
    slots = outgoing.shape[1]
    delta = gathered[0]
    for j in range(1, gathered.shape[0]):
        delta = delta + gathered[j]
    hidden_state = (tokens[...].astype(F32) + delta).astype(BF16)
    hidden[...] = hidden_state
    normed = rms_norm(hidden_state.astype(F32), gain[...])
    sent = dot(select[...].astype(BF16), normed).astype(BF16)
    for x in range(EXPERTS):
        outgoing[x] = sent[x * slots : (x + 1) * slots]


def hidden_kernel(received, gate, up, hidden):
    rows = jnp.concatenate([received[x] for x in range(received.shape[0])], axis=0)
    gate_pre = dot(rows, gate[...])
    up_pre = dot(rows, up[...])
    hidden[...] = (jax.nn.silu(gate_pre) * up_pre).astype(BF16)


def down_kernel(hidden, down, out):
    units = hidden.shape[2]
    total = dot(hidden[0], down[:units])
    for j in range(1, hidden.shape[0]):
        total = total + dot(hidden[j], down[j * units : (j + 1) * units])
    rounded = total.astype(BF16)
    slots = out.shape[1]
    for x in range(out.shape[0]):
        out[x] = rounded[x * slots : (x + 1) * slots]


def combine_kernel(start, returned, table, hidden, mixed):
    quarter = mixed.shape[1]
    rows = jnp.concatenate([returned[x] for x in range(returned.shape[0])], axis=0)
    routed = lax.dot_general(
        table[...],
        rows.astype(F32),
        (((0,), (0,)), ((), ())),
        precision=lax.Precision.HIGHEST,
        preferred_element_type=F32,
    )
    first = pl.multiple_of(start[0], 128)
    residual = hidden[:, pl.ds(first, quarter)].astype(F32)
    mixed[...] = (residual + routed).astype(BF16)


def call(kernel, out, args, limit, scalars=0):
    specs = [pl.BlockSpec(memory_space=pltpu.SMEM)] * scalars
    specs = specs + [pl.BlockSpec(memory_space=pltpu.VMEM)] * (len(args) - scalars)
    return pl.pallas_call(
        kernel,
        out_shape=out,
        in_specs=specs,
        compiler_params=pltpu.CompilerParams(vmem_limit_bytes=limit * MIB),
    )(*args)


def shards(
    tokens,
    norm_gain,
    in_weight,
    decay_rate,
    frequency,
    log_step,
    input_real,
    input_imag,
    output_real,
    output_imag,
    skip_gain,
    state_real,
    state_imag,
    out_weight,
    ffn_gain,
    expert_ids,
    route_weights,
    gate_weight,
    up_weight,
    down_weight,
):
    count, width = tokens.shape
    groups, states = decay_rate.shape
    channels = in_weight.shape[1]
    quarter = down_weight.shape[1]
    flat_state = (count * groups, states)
    struct = jax.ShapeDtypeStruct
    slots = count // 2
    base = jnp.reshape(lax.axis_index("ep") * count, (1,)).astype(jnp.int32)
    start = jnp.reshape(lax.axis_index("tp") * quarter, (1,)).astype(jnp.int32)
    sources = (
        tokens,
        norm_gain.reshape(-1, 128),
        in_weight,
        decay_rate,
        frequency,
        log_step[None],
        jnp.swapaxes(input_real, 1, 2).reshape(channels, states),
        jnp.swapaxes(input_imag, 1, 2).reshape(channels, states),
        output_real.reshape(channels, states),
        output_imag.reshape(channels, states),
        skip_gain[None],
        state_real.reshape(flat_state),
        state_imag.reshape(flat_state),
        ffn_gain.reshape(-1, 128),
        expert_ids.T,
        route_weights.T,
        out_weight,
    )
    hbm = pl.BlockSpec(memory_space=pltpu.HBM)
    vmem = pl.BlockSpec(memory_space=pltpu.VMEM)
    smem = pl.BlockSpec(memory_space=pltpu.SMEM)
    table_shape = struct((EXPERTS * slots, count), F32)
    partial, new_real, new_imag, kept_tokens, kept_gain, select, table = pl.pallas_call(
        mixer_kernel,
        out_shape=(
            struct((count, width), F32),
            struct(flat_state, F32),
            struct(flat_state, F32),
            struct((count, width), BF16),
            struct((1, width), F32),
            table_shape,
            table_shape,
        ),
        in_specs=[smem] + [hbm] * len(sources),
        scratch_shapes=[pltpu.VMEM(v.shape, v.dtype) for v in sources]
        + [pltpu.SemaphoreType.DMA((len(sources),))],
        compiler_params=pltpu.CompilerParams(vmem_limit_bytes=10 * MIB),
    )(base, *[pltpu.with_memory_space_constraint(v, pltpu.HBM) for v in sources])
    gathered = lax.all_gather(partial, "tp")
    outgoing, hidden_state = pl.pallas_call(
        dispatch_kernel,
        out_shape=(struct((EXPERTS, slots, width), BF16), struct((count, width), BF16)),
        in_specs=[vmem] * 4 + [hbm] * 2,
        compiler_params=pltpu.CompilerParams(vmem_limit_bytes=4 * MIB),
    )(
        gathered,
        kept_tokens,
        kept_gain,
        select,
        pltpu.with_memory_space_constraint(gate_weight, pltpu.HBM),
        pltpu.with_memory_space_constraint(up_weight, pltpu.HBM),
    )
    span = lax.axis_size("ep") // EXPERTS
    if span > 1:
        outgoing = jnp.repeat(outgoing, span, axis=0)
    received = lax.all_to_all(outgoing, "ep", split_axis=0, concat_axis=0, tiled=True)
    peers = received.shape[0]
    hidden = call(
        hidden_kernel,
        struct((peers * slots, gate_weight.shape[1]), BF16),
        (received, gate_weight, up_weight),
        4,
    )
    out = call(
        down_kernel,
        struct((peers, slots, quarter), BF16),
        (lax.all_gather(hidden, "tp"), down_weight),
        6,
    )
    returned = lax.all_to_all(out, "ep", split_axis=0, concat_axis=0, tiled=True)
    if span > 1:
        returned = returned.astype(F32).reshape(EXPERTS, span, slots, quarter).sum(axis=1)
    mixed = call(
        combine_kernel,
        struct((count, quarter), BF16),
        (start, returned, table, hidden_state),
        2,
        1,
    )
    shape = state_real.shape
    return (mixed, new_real.reshape(shape), new_imag.reshape(shape))

def solution(mesh):
    in_specs = (
        P("ep", None),
        P(),
        P(None, "tp"),
        P("tp", None),
        P("tp", None),
        P("tp"),
        P("tp", None, None),
        P("tp", None, None),
        P("tp", None, None),
        P("tp", None, None),
        P("tp"),
        P("ep", "tp", None),
        P("ep", "tp", None),
        P("tp", None),
        P(),
        P(),
        P("ep", None),
        P(None, ("ep", "tp")),
        P(None, ("ep", "tp")),
        P("ep", "tp"),
    )
    out_specs = (P("ep", "tp"), P("ep", "tp", None), P("ep", "tp", None))
    return jax.shard_map(shards, mesh=mesh, in_specs=in_specs, out_specs=out_specs, check_vma=False)
```
